32 devices in a mesh: grp: 2 (over x), st: 4 (over y, core), tp: 4 (over z).
Axes of the slice: x: 2, y: 2, z: 4, core: 2. Of those that a mesh axis runs over, the one named last changes fastest.
Arguments:
- tokens: bfloat16 [2048, 2048], P(('grp', 'st')), parts along dimension 0, may hold values from -6 to 6
- pre_gain: float32 [2048], replicated, may hold values from 0.1 to 1.9
- w_gated: bfloat16 [2048, 1536], P(None, 'tp'), may hold values from -0.125 to 0.125
- w_mixed: bfloat16 [2048, 1536], P(None, 'tp'), may hold values from -0.125 to 0.125
- mix_weight: bfloat16 [8, 128, 128], P('tp'), may hold values from -0.5 to 0.5
- w_query: bfloat16 [2048, 1024], P(None, 'tp'), may hold values from -0.125 to 0.125
- w_gate_mix: bfloat16 [2048, 1536], P(None, 'tp'), may hold values from -0.125 to 0.125
- w_gate_read: bfloat16 [2048, 1024], P(None, 'tp'), may hold values from -0.125 to 0.125
- store: bfloat16 [64, 128, 2048], P(('grp', 'st')), parts along dimension 0, may hold values from -6 to 6
- mem_gain: float32 [2048], replicated, may hold values from 1 to 80
- w_key: bfloat16 [2048, 1024], P(None, 'tp'), may hold values from -0.125 to 0.125
- w_value: bfloat16 [2048, 1024], P(None, 'tp'), may hold values from -0.125 to 0.125
- passage_ids: int32 [32, 4], P(('grp', 'st')), parts along dimension 0, may hold values from 0 to 31, as said below
- w_out_mix: bfloat16 [1536, 2048], P('tp'), may hold values from -0.125 to 0.125
- w_out_read: bfloat16 [1024, 2048], P('tp'), may hold values from -0.125 to 0.125
Outputs:
- mixed_out: bfloat16 [2048, 2048], P(('grp', 'st', 'tp')), parts along dimension 0
The draws below stay inside these ranges and needn't reach their ends.
There are 2 independent parts, one for each index of `grp`. The reference program is written for one: setup_inputs(seed, part) draws one part's arguments, and reference() takes and returns one part's arrays. A program takes and returns all parts, laid end to end along the dimension named above; an argument that names none is the same for every part. Nothing has to cross between parts.
Inputs may be any that keep to these rules, and one draw needn't show every extreme that they name: `passage_ids`: passage p is held by index p // 8 of st. The 16 entries of one index of st name at most 8 passages held by any one index of st, and that most is reached in every draw.
All inputs are finite; a program needn't handle non-finite values.
Results may differ from the reference program's by a relative error of at most 0.015.
The reference program's roundings to bfloat16 on the way count: a program that leaves them out, or rounds other values in their place, can miss the bound.
Values may be sent and summed in bfloat16 or wider, within the bound.
No kernel may reach another device: no remote copies, remote signals or barrier semaphores. Data moves between devices by JAX's collectives and lax.ppermute only.
A program may use at most 128 MiB of HBM per device.

```python
import jax
import jax.numpy as jnp
from jax import lax

D = 2048
GROUPS = 8
GW = 192
SW = 1536
XH = 8
HD = 128
XW = 1024
SPAN = 128
RBLOCK = 64
NPB = 4
PROWS = 128
PASS_DEV = 8
TOKENS = 1024
PASSAGES = 32
BLOCKS = 16
REQ = 16
CAP = 8
N_TP = 4


def draw_mem_gain(key, part):
    low_end = 1.0
    high_end = 4.0
    unit = jax.random.uniform(key, (D,), jnp.float32)
    return jnp.exp(jnp.log(low_end) + unit * (jnp.log(high_end) - jnp.log(low_end)))


def draw_passage_ids(key, part):
    readers = PASSAGES // PASS_DEV
    key_pop, key_rest = jax.random.split(jax.random.fold_in(key, 17))
    popular = jax.random.randint(key_pop, (readers,), 0, 4)
    slot_count = readers * CAP
    slot_owner = jnp.arange(slot_count, dtype=jnp.int32) // CAP
    slot_copy = jnp.arange(slot_count, dtype=jnp.int32) % CAP

    def one_reader(reader, reader_key):
        key_noise, key_left, key_right, key_order = jax.random.split(reader_key, 4)
        noise = jax.random.randint(key_noise, (slot_count,), 0, 64)
        score = popular[slot_owner] * 64 + noise
        before = slot_owner == (reader + readers - 1) % readers
        across = (slot_owner == (reader + readers // 2) % readers) & (slot_copy == 0)
        score = jnp.where(before | across, 100000, score)
        score = score * 4096 + jnp.arange(slot_count, dtype=jnp.int32)
        ranking = jnp.argsort(-score, stable=True)
        chosen = slot_owner[ranking[:REQ]]
        within = jnp.minimum(jax.random.randint(key_left, (REQ,), 0, PASS_DEV), jax.random.randint(key_right, (REQ,), 0, PASS_DEV))
        picked = (chosen * PASS_DEV + within).astype(jnp.int32)
        return picked[jax.random.permutation(key_order, REQ)]
    reader_keys = jax.random.split(key_rest, readers)
    every = jax.vmap(one_reader)(jnp.arange(readers, dtype=jnp.int32), reader_keys)
    return every.reshape(BLOCKS, NPB).astype(jnp.int32)


def block_levels(rng, shape, cuts, low, top_value):
    def one(position, parts):
        draws = jax.random.uniform(jax.random.fold_in(jax.random.fold_in(rng, 6), position), (parts,), jnp.float32, low / len(cuts), top_value / len(cuts))
        return jnp.repeat(jnp.exp(draws), shape[position] // parts).reshape((-1,) + (1,) * (len(shape) - position - 1))

    loudness = one(*cuts[0])
    for cut in cuts[1:]:
        loudness = loudness * one(*cut)
    return loudness


def gaussian(key, extent, scale, bound, pieces=(), held_as=jnp.bfloat16):
    result = scale * jax.random.normal(key, extent, jnp.float32)
    if pieces:
        result = result * block_levels(key, extent, pieces, -0.22, 0.18)
    return jnp.clip(result, -bound, bound).astype(held_as)


def setup_inputs(seed: int = 0, part: int = 0) -> dict:
    key_list = jax.random.split(jax.random.key(seed), 16)
    part_keys = jax.random.split(jax.random.fold_in(key_list[15], part), 16)
    tokens = gaussian(part_keys[0], (TOKENS, D), 1.0, 6.0, ((0, 4),))
    pre_gain = jnp.clip(1.0 + 0.18 * jax.random.normal(key_list[1], (D,), jnp.float32), 0.1, 1.9)
    w_gated = gaussian(key_list[2], (D, SW), D ** -0.5, 0.125, ((1, 4),))
    w_mixed = gaussian(key_list[3], (D, SW), D ** -0.5, 0.125, ((1, 4),))
    mix_weight = gaussian(key_list[4], (GROUPS, SPAN, SPAN), SPAN ** -0.5, 0.5, ((0, 4),))
    w_query = gaussian(key_list[5], (D, XW), D ** -0.5, 0.125, ((1, 4),))
    w_gate_mix = gaussian(key_list[6], (D, SW), D ** -0.5, 0.125, ((1, 4),))
    w_gate_read = gaussian(key_list[7], (D, XW), D ** -0.5, 0.125, ((1, 4),))
    store = gaussian(part_keys[8], (PASSAGES, PROWS, D), 1.0, 6.0, ((0, 4),))
    mem_gain = draw_mem_gain(jax.random.fold_in(key_list[15], 71), part)
    w_key = gaussian(key_list[10], (D, XW), D ** -0.5, 0.125, ((1, 4),))
    w_value = gaussian(key_list[11], (D, XW), D ** -0.5, 0.125, ((1, 4),))
    passage_ids = draw_passage_ids(jax.random.fold_in(jax.random.fold_in(key_list[15], part), 71), part)
    w_out_mix = gaussian(key_list[13], (SW, D), (SW + XW) ** -0.5, 0.125, ((0, 4),))
    w_out_read = gaussian(key_list[14], (XW, D), (SW + XW) ** -0.5, 0.125, ((0, 4),))
    return dict(tokens=tokens, pre_gain=pre_gain, w_gated=w_gated, w_mixed=w_mixed, mix_weight=mix_weight, w_query=w_query, w_gate_mix=w_gate_mix, w_gate_read=w_gate_read, store=store, mem_gain=mem_gain, w_key=w_key, w_value=w_value, passage_ids=passage_ids, w_out_mix=w_out_mix, w_out_read=w_out_read)


eps = 1e-06

def reference(tokens, pre_gain, w_gated, w_mixed, mix_weight, w_query, w_gate_mix, w_gate_read, store, mem_gain, w_key, w_value, passage_ids, w_out_mix, w_out_read):
    inputs = tokens.astype(jnp.float32)
    normed = (inputs * lax.rsqrt(lax.optimization_barrier(jnp.mean(inputs * inputs, axis=-1, keepdims=True)) + eps) * pre_gain).astype(jnp.bfloat16)
    gated = jnp.dot(normed, w_gated, preferred_element_type=jnp.float32)
    mixed_in = jnp.dot(normed, w_mixed, preferred_element_type=jnp.float32)
    grouped = mixed_in.reshape(TOKENS, GROUPS, GW)
    group_mean = lax.optimization_barrier(jnp.mean(grouped, axis=-1, keepdims=True))
    centred = grouped - group_mean
    group_var = lax.optimization_barrier(jnp.mean(centred * centred, axis=-1, keepdims=True))
    mixed_norm = (centred * lax.rsqrt(group_var + eps)).astype(jnp.bfloat16)
    causal = jnp.tril(jnp.ones((SPAN, SPAN), dtype=bool))
    mix_masked = jnp.where(causal[None], mix_weight.astype(jnp.float32), 0.0)
    blocked = mixed_norm.reshape(TOKENS // SPAN, SPAN, GROUPS, GW).astype(jnp.float32)
    spatial = jnp.einsum('hts,nshd->nthd', mix_masked, blocked).reshape(TOKENS, SW)
    branch_mix = gated * spatial
    query = jnp.dot(normed, w_query, preferred_element_type=jnp.float32).astype(jnp.bfloat16)
    read_rows = store[passage_ids.reshape(-1)].astype(jnp.float32)
    passage_norm = (read_rows * lax.rsqrt(lax.optimization_barrier(jnp.mean(read_rows * read_rows, axis=-1, keepdims=True)) + eps) * mem_gain).astype(jnp.bfloat16)
    flat_rows = passage_norm.reshape(-1, D)
    keys = jnp.dot(flat_rows, w_key, preferred_element_type=jnp.float32).astype(jnp.bfloat16).reshape(BLOCKS, NPB * PROWS, XH, HD)
    values = jnp.dot(flat_rows, w_value, preferred_element_type=jnp.float32).astype(jnp.bfloat16).reshape(BLOCKS, NPB * PROWS, XH, HD)
    query_blocks = query.reshape(BLOCKS, RBLOCK, XH, HD).astype(jnp.float32)
    scores = jnp.einsum('btha,bkha->bhtk', query_blocks, keys.astype(jnp.float32)) * HD ** (-0.5)
    probs = jax.nn.softmax(scores, axis=-1).astype(jnp.bfloat16)
    branch_read = jnp.einsum('bhtk,bkha->btha', probs.astype(jnp.float32), values.astype(jnp.float32)).reshape(TOKENS, XW)
    gate_mix = jnp.dot(normed, w_gate_mix, preferred_element_type=jnp.float32)
    gate_read = jnp.dot(normed, w_gate_read, preferred_element_type=jnp.float32)
    out_mix = (branch_mix * jax.nn.silu(gate_mix)).astype(jnp.bfloat16)
    out_read = (branch_read * jax.nn.silu(gate_read)).astype(jnp.bfloat16)
    mix_cols = SW // N_TP
    read_cols = XW // N_TP
    total = jnp.zeros((TOKENS, D), jnp.float32)
    for shard in range(N_TP):
        partial_value = jnp.dot(out_mix[:, shard * mix_cols:(shard + 1) * mix_cols], w_out_mix[shard * mix_cols:(shard + 1) * mix_cols], preferred_element_type=jnp.float32)
        partial_value = partial_value + jnp.dot(out_read[:, shard * read_cols:(shard + 1) * read_cols], w_out_read[shard * read_cols:(shard + 1) * read_cols], preferred_element_type=jnp.float32)
        total = total + lax.optimization_barrier(partial_value.astype(jnp.bfloat16)).astype(jnp.float32)
    return total.astype(jnp.bfloat16)
```

```python
import functools

import jax
import jax.numpy as jnp
from jax import lax
from jax.experimental import pallas as pl
from jax.experimental.pallas import tpu as pltpu
from jax.sharding import PartitionSpec as P

HD = 128
SPAN = 128
RBLOCK = 64
PROWS = 128
FAR = -1e30
STAT_ROWS = 16

eps = 1e-06
f32 = jnp.float32
bf16 = jnp.bfloat16


def row_norm(values_in, gain):
    widened = values_in.astype(f32)
    return (
        widened * lax.rsqrt(jnp.mean(widened * widened, axis=-1, keepdims=True) + eps) * gain
    ).astype(bf16)


def pieces_of(row):
    high = row.astype(bf16).astype(f32)
    rest = row - high
    mid = rest.astype(bf16).astype(f32)
    low = (rest - mid).astype(bf16).astype(f32)
    return high, mid, low


def attend_kernel(ids_ref, q_ref, k_ref, v_ref, out_ref, *, held):
    rows, width = q_ref.shape
    base = lax.axis_index("st") * held
    passage = lax.broadcasted_iota(jnp.int32, (held, rows), 0)
    block = lax.broadcasted_iota(jnp.int32, (held, rows), 1) // RBLOCK
    count = jnp.zeros((held, rows), f32)
    for b in range(ids_ref.shape[0]):
        for j in range(ids_ref.shape[1]):
            hit = (passage == ids_ref[b, j] - base) & (block == b)
            count = count + jnp.where(hit, 1.0, 0.0)
    bias = jnp.where(count > 0.0, jnp.log(jnp.maximum(count, 1.0)), FAR)
    which = lax.broadcasted_iota(jnp.int32, (STAT_ROWS, rows), 0)
    stats = jnp.zeros((STAT_ROWS, rows), f32)
    for h in range(width // HD):
        cols = slice(h * HD, (h + 1) * HD)
        scores = lax.dot_general(
            k_ref[:, cols], q_ref[:, cols], (((1,), (1,)), ((), ())), preferred_element_type=f32
        ) * HD ** (-0.5)
        shifted = scores.reshape(held, PROWS, rows) + bias[:, None, :]
        top = jnp.max(jnp.max(shifted, axis=0), axis=0, keepdims=True)
        weights = jnp.exp(shifted - top[None])
        total = jnp.sum(jnp.sum(weights, axis=0), axis=0, keepdims=True)
        read = lax.dot_general(
            weights.astype(bf16).reshape(held * PROWS, rows),
            v_ref[:, cols],
            (((0,), (0,)), ((), ())),
            preferred_element_type=f32,
        )
        out_ref[:rows, cols] = read.astype(bf16)
        for i, piece in enumerate(pieces_of(top) + pieces_of(total)):
            stats = jnp.where(which == h * 6 + i, piece, stats)
    if rows == width:
        out_ref[rows:, :] = stats.astype(bf16)
    else:
        for part in range(rows // width):
            start = rows + part * STAT_ROWS
            out_ref[start : start + STAT_ROWS, :] = stats[:, part * width : (part + 1) * width].astype(bf16)


def attend(ids, query, keys, values, held):
    rows, width = query.shape
    return pl.pallas_call(
        functools.partial(attend_kernel, held=held),
        out_shape=jax.ShapeDtypeStruct((rows + STAT_ROWS * (rows // width), width), bf16),
        in_specs=[pl.BlockSpec(memory_space=pltpu.SMEM)] + [pl.BlockSpec(memory_space=pltpu.VMEM)] * 3,
        out_specs=pl.BlockSpec(memory_space=pltpu.VMEM),
        cost_estimate=pl.CostEstimate(
            flops=4 * rows * keys.shape[0] * width,
            transcendentals=rows * keys.shape[0] * (width // HD),
            bytes_accessed=2 * (2 * keys.size + 2 * query.size),
        ),
        name="attend",
    )(ids, query, keys, values)


def mix_kernel(mixed_ref, gated_ref, gate_ref, mixw_ref, out_ref):
    rows, width = mixed_ref.shape
    groups = mixw_ref.shape[0]
    group_width = width // groups
    mixed = mixed_ref[...]
    lane = lax.broadcasted_iota(jnp.int32, (1, width), 1) // group_width
    inside = [lane == g for g in range(groups)]

    def group_mean(value):
        result = jnp.zeros_like(value)
        for g in range(groups):
            mean = jnp.sum(jnp.where(inside[g], value, 0.0), axis=-1, keepdims=True) / group_width
            result = jnp.where(inside[g], mean, result)
        return result

    centred = mixed - group_mean(mixed)
    normal = (centred * lax.rsqrt(group_mean(centred * centred) + eps)).astype(bf16)
    below = lax.broadcasted_iota(jnp.int32, (SPAN, SPAN), 0) >= lax.broadcasted_iota(
        jnp.int32, (SPAN, SPAN), 1
    )
    masked = [jnp.where(below, mixw_ref[g].astype(f32), 0.0).astype(bf16) for g in range(groups)]
    for n in range(rows // SPAN):
        part = slice(n * SPAN, (n + 1) * SPAN)
        spatial = jnp.zeros((SPAN, width), f32)
        for g in range(groups):
            spatial = jnp.where(
                inside[g], jnp.dot(masked[g], normal[part], preferred_element_type=f32), spatial
            )
        gate = gate_ref[part, :]
        out_ref[part, :] = (gated_ref[part, :] * spatial * (gate / (1.0 + jnp.exp(-gate)))).astype(bf16)


def mix(mixed_in, gated, gate_mix, mix_weight):
    return pl.pallas_call(
        mix_kernel,
        out_shape=jax.ShapeDtypeStruct(mixed_in.shape, bf16),
        in_specs=[pl.BlockSpec(memory_space=pltpu.VMEM)] * 4,
        out_specs=pl.BlockSpec(memory_space=pltpu.VMEM),
        cost_estimate=pl.CostEstimate(
            flops=2 * mixed_in.size * SPAN * mix_weight.shape[0] + 20 * mixed_in.size,
            transcendentals=mixed_in.size,
            bytes_accessed=14 * mixed_in.size,
        ),
        name="mix",
    )(mixed_in, gated, gate_mix, mix_weight)


def finish_kernel(*refs, owners, shares):
    parts = refs[:owners]
    gate_ref, mix_ref, w_mix_ref, w_read_ref = refs[owners : owners + 4]
    outs = refs[owners + 4 : owners + 4 + shares]
    whole_ref = refs[owners + 4 + shares]
    rows, width = gate_ref.shape
    heads = width // HD
    stats = []
    for part in parts:
        pieces = [
            part[rows + i * STAT_ROWS : rows + (i + 1) * STAT_ROWS, :].astype(f32)
            for i in range(rows // width)
        ]
        stats.append(pieces[0] if len(pieces) == 1 else jnp.concatenate(pieces, axis=1))

    def value_of(stat, row):
        return stat[row : row + 1] + stat[row + 1 : row + 2] + stat[row + 2 : row + 3]

    for h in range(heads):
        cols = slice(h * HD, (h + 1) * HD)
        tops = [value_of(stat, h * 6) for stat in stats]
        highest = functools.reduce(jnp.maximum, tops)
        scales = [jnp.exp(top - highest) for top in tops]
        total = sum(scale * value_of(stat, h * 6 + 3) for scale, stat in zip(scales, stats))
        shares_of = [scale / total for scale in scales]
        padding = (-len(shares_of)) % 8
        square = jnp.concatenate(shares_of + [jnp.zeros((padding, rows), f32)] * (padding > 0), axis=0)
        columns = jnp.transpose(square)
        read = jnp.zeros((rows, HD), f32)
        for i, part in enumerate(parts):
            read = read + columns[:, i : i + 1] * part[:rows, cols].astype(f32)
        gate = gate_ref[:, cols]
        gated = (read * (gate / (1.0 + jnp.exp(-gate)))).astype(bf16)
        if h == 0:
            total_read = [gated]
        else:
            total_read.append(gated)
    out_read = total_read[0] if heads == 1 else jnp.concatenate(total_read, axis=1)
    partial = jnp.dot(mix_ref[...], w_mix_ref[...], preferred_element_type=f32) + jnp.dot(
        out_read, w_read_ref[...], preferred_element_type=f32
    )
    whole_ref[...] = partial.astype(bf16)
    here = lax.axis_index("tp")
    share_rows = rows // shares
    for k in range(shares):
        start = pl.multiple_of(((here + k) % shares) * share_rows, share_rows)
        outs[k][...] = whole_ref[pl.ds(start, share_rows), :]


def finish(parts, gate_read, out_mix, w_out_mix, w_out_read, shares):
    rows = gate_read.shape[0]
    model = w_out_mix.shape[1]
    share = jax.ShapeDtypeStruct((rows // shares, model), bf16)
    return pl.pallas_call(
        functools.partial(finish_kernel, owners=len(parts), shares=shares),
        out_shape=[share] * shares,
        in_specs=[pl.BlockSpec(memory_space=pltpu.VMEM)] * (len(parts) + 4),
        out_specs=[pl.BlockSpec(memory_space=pltpu.VMEM)] * shares,
        scratch_shapes=[pltpu.VMEM((rows, model), bf16)],
        cost_estimate=pl.CostEstimate(
            flops=2 * rows * model * (w_out_mix.shape[0] + w_out_read.shape[0]),
            transcendentals=gate_read.size,
            bytes_accessed=2 * (w_out_mix.size + w_out_read.size + rows * model),
        ),
        name="finish",
    )(*parts, gate_read, out_mix, w_out_mix, w_out_read)


def shifted_by(value, axis, step):
    count = lax.axis_size(axis)
    if step % count == 0:
        return value
    return lax.ppermute(value, axis, [(i, (i + step) % count) for i in range(count)])


def local(
    tokens,
    pre_gain,
    w_gated,
    w_mixed,
    mix_weight,
    w_query,
    w_gate_mix,
    w_gate_read,
    store,
    mem_gain,
    w_key,
    w_value,
    passage_ids,
    w_out_mix,
    w_out_read,
):
    readers = lax.axis_size("st")
    shares = lax.axis_size("tp")
    held = store.shape[0]
    ids = [shifted_by(passage_ids, "st", k) for k in range(readers)]
    normed = lax.optimization_barrier(row_norm(tokens, pre_gain))
    query = jnp.dot(normed, w_query, preferred_element_type=f32).astype(bf16)
    queries = [shifted_by(query, "st", k) for k in range(readers)]
    held_rows = lax.optimization_barrier(row_norm(store, mem_gain).reshape(-1, store.shape[-1]))
    keys = jnp.dot(held_rows, w_key, preferred_element_type=f32).astype(bf16)
    values = jnp.dot(held_rows, w_value, preferred_element_type=f32).astype(bf16)
    parts = [None] * readers
    for k in list(range(1, readers)) + [0]:
        parts[k] = shifted_by(attend(ids[k], queries[k], keys, values, held), "st", -k)
    gated = jnp.dot(normed, w_gated, preferred_element_type=f32)
    mixed_in = jnp.dot(normed, w_mixed, preferred_element_type=f32)
    gate_mix = jnp.dot(normed, w_gate_mix, preferred_element_type=f32)
    gate_read = jnp.dot(normed, w_gate_read, preferred_element_type=f32)
    out_mix = mix(mixed_in, gated, gate_mix, mix_weight)
    chunks = finish(parts, gate_read, out_mix, w_out_mix, w_out_read, shares)
    arrived = [shifted_by(chunks[k], "tp", k) for k in range(shares)]
    return functools.reduce(jnp.add, [part.astype(f32) for part in arrived]).astype(bf16)


def solution(mesh):
    placed = (
        P(("grp", "st"), None),
        P(),
        P(None, "tp"),
        P(None, "tp"),
        P("tp", None, None),
        P(None, "tp"),
        P(None, "tp"),
        P(None, "tp"),
        P(("grp", "st"), None, None),
        P(),
        P(None, "tp"),
        P(None, "tp"),
        P(("grp", "st"), None),
        P("tp", None),
        P("tp", None),
    )
    return jax.shard_map(
        local, mesh=mesh, in_specs=placed, out_specs=P(("grp", "st", "tp"), None), check_vma=False
    )
```

```python
import functools

import jax
import jax.numpy as jnp
from jax import lax
from jax.experimental import pallas as pl
from jax.experimental.pallas import tpu as pltpu
from jax.sharding import PartitionSpec as P

HD = 128
SPAN = 128
RBLOCK = 64
PROWS = 128
FAR = -1e30
EXTRA = 16
NPB = 4

eps = 1e-06
f32 = jnp.float32
bf16 = jnp.bfloat16


LOG2E = 1.4426950408889634


def row_norm(values_in, gain):
    widened = values_in.astype(f32)
    return (
        widened * lax.rsqrt(jnp.mean(widened * widened, axis=-1, keepdims=True) + eps) * gain
    ).astype(bf16)


def pieces_of(row):
    high = row.astype(bf16).astype(f32)
    rest = row - high
    mid = rest.astype(bf16).astype(f32)
    low = (rest - mid).astype(bf16).astype(f32)
    return high, mid, low


def silu(gate):
    return gate / (1.0 + jnp.exp(-gate))


def query_kernel(first_ref, ids_ref, tokens_ref, gain_ref, w_ref, normed_ref, query_ref, *, held):
    rows = tokens_ref.shape[0]
    normed = row_norm(tokens_ref[...], gain_ref[...])
    normed_ref[...] = normed
    query_ref[:rows, :] = jnp.dot(normed, w_ref[...], preferred_element_type=f32).astype(bf16)
    width = query_ref.shape[1]
    blocks = rows // RBLOCK
    first_block = ((pl.program_id(0) + first_ref[0]) % 2) * blocks
    block = lax.broadcasted_iota(jnp.int32, (EXTRA, width), 1) // RBLOCK
    line = lax.broadcasted_iota(jnp.int32, (EXTRA, width), 0)
    table = jnp.zeros((EXTRA, width), jnp.int32)
    for b in range(blocks):
        for j in range(ids_ref.shape[1]):
            name = ids_ref[first_block + b, j]
            table = jnp.where((block == b) & (line == 2 * j), name // held, table)
            table = jnp.where((block == b) & (line == 2 * j + 1), name % held, table)
    query_ref[rows:, :] = table.astype(f32).astype(bf16)


def make_queries(first, ids, tokens, gain, w_query, held):
    rows, model = tokens.shape
    width = w_query.shape[1]
    half = rows // 2
    return pl.pallas_call(
        functools.partial(query_kernel, held=held),
        grid_spec=pltpu.PrefetchScalarGridSpec(
            num_scalar_prefetch=2,
            grid=(2,),
            in_specs=[
                pl.BlockSpec((half, model), lambda i, first, ids: ((i + first[0]) % 2, 0)),
                pl.BlockSpec((1, model), lambda i, first, ids: (0, 0)),
                pl.BlockSpec((model, width), lambda i, first, ids: (0, 0)),
            ],
            out_specs=[
                pl.BlockSpec((half, model), lambda i, first, ids: (i, 0)),
                pl.BlockSpec((half + EXTRA, width), lambda i, first, ids: (i, 0)),
            ],
        ),
        out_shape=[
            jax.ShapeDtypeStruct((rows, model), bf16),
            jax.ShapeDtypeStruct((rows + 2 * EXTRA, width), bf16),
        ],
        cost_estimate=pl.CostEstimate(
            flops=2 * rows * model * width,
            transcendentals=rows,
            bytes_accessed=2 * (2 * tokens.size + w_query.size),
        ),
        name="queries",
    )(first, ids, tokens, gain.reshape(1, -1), w_query)


def attend_kernel(q_ref, k_ref, v_ref, out_ref, *, held, part):
    rows = out_ref.shape[0] - EXTRA
    width = out_ref.shape[1]
    start = part * (rows + EXTRA)
    here = lax.axis_index("st").astype(f32)
    table = q_ref[start + rows : start + rows + EXTRA, :rows].astype(f32)
    passage = lax.broadcasted_iota(jnp.int32, (held, rows), 0).astype(f32)
    count = jnp.zeros((held, rows), f32)
    for j in range(NPB):
        mine = table[2 * j : 2 * j + 1] == here
        hit = (passage == table[2 * j + 1 : 2 * j + 2]) & mine
        count = count + jnp.where(hit, 1.0, 0.0)
    bias = jnp.where(count > 0.0, jnp.log2(jnp.maximum(count, 1.0)), FAR)
    which = lax.broadcasted_iota(jnp.int32, (EXTRA, rows), 0)
    for h in range(width // HD):
        cols = slice(h * HD, (h + 1) * HD)
        scores = lax.dot_general(
            k_ref[:, cols],
            q_ref[start : start + rows, cols],
            (((1,), (1,)), ((), ())),
            preferred_element_type=f32,
        ) * (HD ** (-0.5) * LOG2E)
        shifted = scores.reshape(held, PROWS, rows) + bias[:, None, :]
        top = jnp.max(jnp.max(shifted, axis=0), axis=0, keepdims=True)
        weights = jnp.exp2(shifted - top[None])
        total = jnp.sum(jnp.sum(weights, axis=0), axis=0, keepdims=True)
        read = lax.dot_general(
            weights.astype(bf16).reshape(held * PROWS, rows),
            v_ref[:, cols],
            (((0,), (0,)), ((), ())),
            preferred_element_type=f32,
        )
        out_ref[:rows, cols] = read.astype(bf16)
        stats = jnp.zeros((EXTRA, rows), f32)
        for i, piece in enumerate(pieces_of(top) + pieces_of(total)):
            stats = jnp.where(which == i, piece, stats)
        out_ref[rows:, h * HD : h * HD + rows] = stats.astype(bf16)


def attend(query, keys, values, held, part):
    rows = query.shape[0] // 2 - EXTRA
    width = query.shape[1]
    assert rows == HD
    return pl.pallas_call(
        functools.partial(attend_kernel, held=held, part=part),
        out_shape=jax.ShapeDtypeStruct((rows + EXTRA, width), bf16),
        in_specs=[pl.BlockSpec(memory_space=pltpu.VMEM)] * 3,
        out_specs=pl.BlockSpec(memory_space=pltpu.VMEM),
        cost_estimate=pl.CostEstimate(
            flops=4 * rows * keys.shape[0] * width,
            transcendentals=rows * keys.shape[0] * (width // HD),
            bytes_accessed=2 * (2 * keys.size + 2 * query.size),
        ),
        name="attend",
    )(query, keys, values)


def mix_kernel(mixed_ref, gated_ref, gate_ref, mixw_ref, out_ref, *, part):
    rows, width = out_ref.shape
    groups = mixw_ref.shape[0]
    group_width = width // groups
    start = part * rows
    mixed = mixed_ref[start : start + rows, :]
    lane = lax.broadcasted_iota(jnp.int32, (1, width), 1) // group_width
    inside = [lane == g for g in range(groups)]

    def group_mean(value):
        result = jnp.zeros_like(value)
        for g in range(groups):
            mean = jnp.sum(jnp.where(inside[g], value, 0.0), axis=-1, keepdims=True) / group_width
            result = jnp.where(inside[g], mean, result)
        return result

    centred = mixed - group_mean(mixed)
    normal = (centred * lax.rsqrt(group_mean(centred * centred) + eps)).astype(bf16)
    below = lax.broadcasted_iota(jnp.int32, (SPAN, SPAN), 0) >= lax.broadcasted_iota(
        jnp.int32, (SPAN, SPAN), 1
    )
    masked = [jnp.where(below, mixw_ref[g].astype(f32), 0.0).astype(bf16) for g in range(groups)]
    for n in range(rows // SPAN):
        block = slice(n * SPAN, (n + 1) * SPAN)
        source = slice(start + n * SPAN, start + (n + 1) * SPAN)
        spatial = jnp.zeros((SPAN, width), f32)
        for g in range(groups):
            spatial = jnp.where(
                inside[g], jnp.dot(masked[g], normal[block], preferred_element_type=f32), spatial
            )
        out_ref[block, :] = (gated_ref[source, :] * spatial * silu(gate_ref[source, :])).astype(bf16)


def mix(mixed_in, gated, gate_mix, mix_weight, part):
    rows, width = mixed_in.shape
    return pl.pallas_call(
        functools.partial(mix_kernel, part=part),
        out_shape=jax.ShapeDtypeStruct((rows // 2, width), bf16),
        in_specs=[pl.BlockSpec(memory_space=pltpu.VMEM)] * 4,
        out_specs=pl.BlockSpec(memory_space=pltpu.VMEM),
        cost_estimate=pl.CostEstimate(
            flops=mixed_in.size * SPAN * mix_weight.shape[0] + 10 * mixed_in.size,
            transcendentals=mixed_in.size // 2,
            bytes_accessed=7 * mixed_in.size,
        ),
        name="mix",
    )(mixed_in, gated, gate_mix, mix_weight)


def finish_kernel(*refs, owners, shares, part):
    parts = refs[:owners]
    gate_ref, mix_ref, w_mix_ref, w_read_ref = refs[owners : owners + 4]
    outs = refs[owners + 4 : owners + 4 + shares]
    whole_ref = refs[owners + 4 + shares]
    rows = mix_ref.shape[0]
    width = gate_ref.shape[1]
    out_read = []
    for h in range(width // HD):
        cols = slice(h * HD, (h + 1) * HD)
        stats = [p[rows:, h * HD : h * HD + rows].astype(f32) for p in parts]
        tops = [stat[0:1] + stat[1:2] + stat[2:3] for stat in stats]
        totals = [stat[3:4] + stat[4:5] + stat[5:6] for stat in stats]
        highest = functools.reduce(jnp.maximum, tops)
        scales = [jnp.exp2(top - highest) for top in tops]
        whole = sum(scale * total for scale, total in zip(scales, totals))
        weights = [scale / whole for scale in scales]
        padding = (-len(weights)) % 8
        square = jnp.concatenate(weights + [jnp.zeros((padding, rows), f32)] * (padding > 0), axis=0)
        columns = jnp.transpose(square)
        read = jnp.zeros((rows, HD), f32)
        for i, p in enumerate(parts):
            read = read + columns[:, i : i + 1] * p[:rows, cols].astype(f32)
        out_read.append((read * silu(gate_ref[part * rows : (part + 1) * rows, cols])).astype(bf16))
    out_read = out_read[0] if len(out_read) == 1 else jnp.concatenate(out_read, axis=1)
    partial = jnp.dot(mix_ref[...], w_mix_ref[...], preferred_element_type=f32) + jnp.dot(
        out_read, w_read_ref[...], preferred_element_type=f32
    )
    whole_ref[...] = partial.astype(bf16)
    here = lax.axis_index("tp")
    share_rows = rows // shares
    for k in range(shares):
        start = pl.multiple_of((jnp.bitwise_xor(here, k) % shares) * share_rows, share_rows)
        outs[k][...] = whole_ref[pl.ds(start, share_rows), :]


def finish(parts, gate_read, out_mix, w_out_mix, w_out_read, shares, part):
    rows = out_mix.shape[0]
    model = w_out_mix.shape[1]
    share = jax.ShapeDtypeStruct((rows // shares, model), bf16)
    return pl.pallas_call(
        functools.partial(finish_kernel, owners=len(parts), shares=shares, part=part),
        out_shape=[share] * shares,
        in_specs=[pl.BlockSpec(memory_space=pltpu.VMEM)] * (len(parts) + 4),
        out_specs=[pl.BlockSpec(memory_space=pltpu.VMEM)] * shares,
        scratch_shapes=[pltpu.VMEM((rows, model), bf16)],
        cost_estimate=pl.CostEstimate(
            flops=2 * rows * model * (w_out_mix.shape[0] + w_out_read.shape[0]),
            transcendentals=gate_read.size,
            bytes_accessed=2 * (w_out_mix.size + w_out_read.size + rows * model),
        ),
        name="finish",
    )(*parts, gate_read, out_mix, w_out_mix, w_out_read)


def shifted_by(value, axis, step):
    count = lax.axis_size(axis)
    if step % count == 0:
        return value
    return lax.ppermute(value, axis, [(i, (i + step) % count) for i in range(count)])


def crossed_by(value, axis, mask):
    if mask == 0:
        return value
    return lax.ppermute(value, axis, [(i, i ^ mask) for i in range(lax.axis_size(axis))])


def local(
    tokens,
    pre_gain,
    w_gated,
    w_mixed,
    mix_weight,
    w_query,
    w_gate_mix,
    w_gate_read,
    store,
    mem_gain,
    w_key,
    w_value,
    passage_ids,
    w_out_mix,
    w_out_read,
):
    readers = lax.axis_size("st")
    near = lax.axis_size("tp") // 2
    held = store.shape[0]
    first = (1 - lax.axis_index("tp") // near).astype(jnp.int32).reshape(1)
    normed, query = make_queries(first, passage_ids, tokens, pre_gain, w_query, held)
    queries = [shifted_by(query, "st", k) for k in range(readers)]
    held_rows = lax.optimization_barrier(row_norm(store, mem_gain).reshape(-1, store.shape[-1]))
    keys = jnp.dot(held_rows, w_key, preferred_element_type=f32).astype(bf16)
    values = jnp.dot(held_rows, w_value, preferred_element_type=f32).astype(bf16)
    gated = jnp.dot(normed, w_gated, preferred_element_type=f32)
    mixed_in = jnp.dot(normed, w_mixed, preferred_element_type=f32)
    gate_mix = jnp.dot(normed, w_gate_mix, preferred_element_type=f32)
    gate_read = jnp.dot(normed, w_gate_read, preferred_element_type=f32)
    arrived = []
    for part in range(2):
        reads = [None] * readers
        for k in list(range(1, readers)) + [0]:
            reads[k] = shifted_by(attend(queries[k], keys, values, held, part), "st", -k)
        out_mix = mix(mixed_in, gated, gate_mix, mix_weight, part)
        chunks = finish(reads, gate_read, out_mix, w_out_mix, w_out_read, near, part)
        base = near * (1 - part)
        arrived += [crossed_by(chunks[k], "tp", base + k) for k in range(near)]
    return functools.reduce(jnp.add, [piece.astype(f32) for piece in arrived]).astype(bf16)


def solution(mesh):
    placed = (
        P(("grp", "st"), None),
        P(),
        P(None, "tp"),
        P(None, "tp"),
        P("tp", None, None),
        P(None, "tp"),
        P(None, "tp"),
        P(None, "tp"),
        P(("grp", "st"), None, None),
        P(),
        P(None, "tp"),
        P(None, "tp"),
        P(("grp", "st"), None),
        P("tp", None),
        P("tp", None),
    )
    return jax.shard_map(
        local, mesh=mesh, in_specs=placed, out_specs=P(("grp", "st", "tp"), None), check_vma=False
    )
```

```python
import functools

import jax
import jax.numpy as jnp
from jax import lax
from jax.experimental import pallas as pl
from jax.experimental.pallas import tpu as pltpu
from jax.sharding import PartitionSpec as P

HD = 128
SPAN = 128
RBLOCK = 64
PROWS = 128
FAR = -1e30
EXTRA = 16
NPB = 4

eps = 1e-06
f32 = jnp.float32
bf16 = jnp.bfloat16


LOG2E = 1.4426950408889634


def row_norm(values_in, gain):
    widened = values_in.astype(f32)
    return (
        widened * lax.rsqrt(jnp.mean(widened * widened, axis=-1, keepdims=True) + eps) * gain
    ).astype(bf16)


def pieces_of(row):
    high = row.astype(bf16).astype(f32)
    rest = row - high
    mid = rest.astype(bf16).astype(f32)
    low = (rest - mid).astype(bf16).astype(f32)
    return high, mid, low


def silu(gate):
    return gate / (1.0 + jnp.exp(-gate))


def query_kernel(first_ref, ids_ref, tokens_ref, gain_ref, w_ref, normed_ref, query_ref, *, held):
    rows = tokens_ref.shape[0]
    normed = row_norm(tokens_ref[...], gain_ref[...])
    normed_ref[...] = normed
    query_ref[:rows, :] = jnp.dot(normed, w_ref[...], preferred_element_type=f32).astype(bf16)
    width = query_ref.shape[1]
    blocks = rows // RBLOCK
    first_block = ((pl.program_id(0) + first_ref[0]) % 2) * blocks
    block = lax.broadcasted_iota(jnp.int32, (EXTRA, width), 1) // RBLOCK
    line = lax.broadcasted_iota(jnp.int32, (EXTRA, width), 0)
    table = jnp.zeros((EXTRA, width), jnp.int32)
    for b in range(blocks):
        for j in range(ids_ref.shape[1]):
            name = ids_ref[first_block + b, j]
            table = jnp.where((block == b) & (line == 2 * j), name // held, table)
            table = jnp.where((block == b) & (line == 2 * j + 1), name % held, table)
    query_ref[rows:, :] = table.astype(f32).astype(bf16)


def make_queries(first, ids, tokens, gain, w_query, held):
    rows, model = tokens.shape
    width = w_query.shape[1]
    half = rows // 2
    return pl.pallas_call(
        functools.partial(query_kernel, held=held),
        grid_spec=pltpu.PrefetchScalarGridSpec(
            num_scalar_prefetch=2,
            grid=(2,),
            in_specs=[
                pl.BlockSpec((half, model), lambda i, first, ids: ((i + first[0]) % 2, 0)),
                pl.BlockSpec((1, model), lambda i, first, ids: (0, 0)),
                pl.BlockSpec((model, width), lambda i, first, ids: (0, 0)),
            ],
            out_specs=[
                pl.BlockSpec((half, model), lambda i, first, ids: (i, 0)),
                pl.BlockSpec((half + EXTRA, width), lambda i, first, ids: (i, 0)),
            ],
        ),
        out_shape=[
            jax.ShapeDtypeStruct((rows, model), bf16),
            jax.ShapeDtypeStruct((rows + 2 * EXTRA, width), bf16),
        ],
        cost_estimate=pl.CostEstimate(
            flops=2 * rows * model * width,
            transcendentals=rows,
            bytes_accessed=2 * (2 * tokens.size + w_query.size),
        ),
        name="queries",
    )(first, ids, tokens, gain.reshape(1, -1), w_query)


def store_kernel(rows_ref, gain_ref, wk_ref, wv_ref, k_ref, v_ref):
    rows = row_norm(rows_ref[...], gain_ref[...])
    k_ref[...] = jnp.dot(rows, wk_ref[...], preferred_element_type=f32).astype(bf16)
    v_ref[...] = jnp.dot(rows, wv_ref[...], preferred_element_type=f32).astype(bf16)


def project_store(store, gain, w_key, w_value):
    model = store.shape[-1]
    flat = store.reshape(-1, model)
    width = w_key.shape[1]
    step = 2 * PROWS
    whole = pl.BlockSpec((model, width), lambda i: (0, 0))
    tile = pl.BlockSpec((step, width), lambda i: (i, 0))
    out = jax.ShapeDtypeStruct((flat.shape[0], width), bf16)
    return pl.pallas_call(
        store_kernel,
        grid=(flat.shape[0] // step,),
        in_specs=[
            pl.BlockSpec((step, model), lambda i: (i, 0)),
            pl.BlockSpec((1, model), lambda i: (0, 0)),
            whole,
            whole,
        ],
        out_specs=[tile, tile],
        out_shape=[out, out],
        cost_estimate=pl.CostEstimate(
            flops=4 * flat.size * width,
            transcendentals=flat.shape[0],
            bytes_accessed=2 * (flat.size + 2 * w_key.size + 2 * flat.shape[0] * width),
        ),
        name="project_store",
    )(flat, gain.reshape(1, -1), w_key, w_value)


def attend_kernel(*refs, readers, held, part):
    queries = refs[:readers]
    k_ref, v_ref = refs[readers : readers + 2]
    outs = refs[readers + 2 :]
    rows = outs[0].shape[0] - EXTRA
    width = outs[0].shape[1]
    start = part * (rows + EXTRA)
    here = lax.axis_index("st").astype(f32)
    passage = lax.broadcasted_iota(jnp.int32, (held, rows), 0).astype(f32)
    which = lax.broadcasted_iota(jnp.int32, (EXTRA, rows), 0)
    for q_ref, out_ref in zip(queries, outs):
        table = q_ref[start + rows : start + rows + EXTRA, :rows].astype(f32)
        count = jnp.zeros((held, rows), f32)
        for j in range(NPB):
            mine = table[2 * j : 2 * j + 1] == here
            hit = (passage == table[2 * j + 1 : 2 * j + 2]) & mine
            count = count + jnp.where(hit, 1.0, 0.0)
        bias = jnp.where(count > 0.0, jnp.log2(jnp.maximum(count, 1.0)), FAR)
        for h in range(width // HD):
            cols = slice(h * HD, (h + 1) * HD)
            scores = lax.dot_general(
                k_ref[:, cols],
                q_ref[start : start + rows, cols],
                (((1,), (1,)), ((), ())),
                preferred_element_type=f32,
            ) * (HD ** (-0.5) * LOG2E)
            shifted = scores.reshape(held, PROWS, rows) + bias[:, None, :]
            top = jnp.max(jnp.max(shifted, axis=0), axis=0, keepdims=True)
            weights = jnp.exp2(shifted - top[None])
            total = jnp.sum(jnp.sum(weights, axis=0), axis=0, keepdims=True)
            read = lax.dot_general(
                weights.astype(bf16).reshape(held * PROWS, rows),
                v_ref[:, cols],
                (((0,), (0,)), ((), ())),
                preferred_element_type=f32,
            )
            out_ref[:rows, cols] = read.astype(bf16)
            stats = jnp.zeros((EXTRA, rows), f32)
            for i, piece in enumerate(pieces_of(top) + pieces_of(total)):
                stats = jnp.where(which == i, piece, stats)
            out_ref[rows:, h * HD : h * HD + rows] = stats.astype(bf16)


def attend(queries, keys, values, held, part):
    readers = len(queries)
    rows = queries[0].shape[0] // 2 - EXTRA
    width = queries[0].shape[1]
    assert rows == HD
    return pl.pallas_call(
        functools.partial(attend_kernel, readers=readers, held=held, part=part),
        out_shape=[jax.ShapeDtypeStruct((rows + EXTRA, width), bf16)] * readers,
        in_specs=[pl.BlockSpec(memory_space=pltpu.VMEM)] * (readers + 2),
        out_specs=[pl.BlockSpec(memory_space=pltpu.VMEM)] * readers,
        cost_estimate=pl.CostEstimate(
            flops=4 * readers * rows * keys.shape[0] * width,
            transcendentals=readers * rows * keys.shape[0] * (width // HD),
            bytes_accessed=2 * (2 * keys.size + 2 * readers * queries[0].size),
        ),
        name="attend",
    )(*queries, keys, values)


def mix_kernel(mixed_ref, gated_ref, gate_ref, mixw_ref, out_ref):
    rows, width = out_ref.shape
    groups = mixw_ref.shape[0]
    group_width = width // groups
    mixed = mixed_ref[...]
    lane = lax.broadcasted_iota(jnp.int32, (1, width), 1) // group_width
    inside = [lane == g for g in range(groups)]

    def group_mean(value):
        result = jnp.zeros_like(value)
        for g in range(groups):
            mean = jnp.sum(jnp.where(inside[g], value, 0.0), axis=-1, keepdims=True) / group_width
            result = jnp.where(inside[g], mean, result)
        return result

    centred = mixed - group_mean(mixed)
    normal = (centred * lax.rsqrt(group_mean(centred * centred) + eps)).astype(bf16)
    below = lax.broadcasted_iota(jnp.int32, (SPAN, SPAN), 0) >= lax.broadcasted_iota(
        jnp.int32, (SPAN, SPAN), 1
    )
    masked = [jnp.where(below, mixw_ref[g].astype(f32), 0.0).astype(bf16) for g in range(groups)]
    for n in range(rows // SPAN):
        block = slice(n * SPAN, (n + 1) * SPAN)
        spatial = jnp.zeros((SPAN, width), f32)
        for g in range(groups):
            spatial = jnp.where(
                inside[g], jnp.dot(masked[g], normal[block], preferred_element_type=f32), spatial
            )
        out_ref[block, :] = (gated_ref[block, :] * spatial * silu(gate_ref[block, :])).astype(bf16)


def mix(mixed_in, gated, gate_mix, mix_weight):
    rows, width = mixed_in.shape
    return pl.pallas_call(
        mix_kernel,
        out_shape=jax.ShapeDtypeStruct((rows, width), bf16),
        in_specs=[pl.BlockSpec(memory_space=pltpu.VMEM)] * 4,
        out_specs=pl.BlockSpec(memory_space=pltpu.VMEM),
        cost_estimate=pl.CostEstimate(
            flops=2 * mixed_in.size * SPAN * mix_weight.shape[0] + 20 * mixed_in.size,
            transcendentals=mixed_in.size,
            bytes_accessed=14 * mixed_in.size,
        ),
        name="mix",
    )(mixed_in, gated, gate_mix, mix_weight)


def finish_kernel(*refs, owners, shares, part):
    parts = refs[:owners]
    gate_ref, mix_ref, w_mix_ref, w_read_ref = refs[owners : owners + 4]
    outs = refs[owners + 4 : owners + 4 + shares]
    whole_ref = refs[owners + 4 + shares]
    rows = mix_ref.shape[0] // 2
    width = gate_ref.shape[1]
    out_read = []
    for h in range(width // HD):
        cols = slice(h * HD, (h + 1) * HD)
        stats = [p[rows:, h * HD : h * HD + rows].astype(f32) for p in parts]
        tops = [stat[0:1] + stat[1:2] + stat[2:3] for stat in stats]
        totals = [stat[3:4] + stat[4:5] + stat[5:6] for stat in stats]
        highest = functools.reduce(jnp.maximum, tops)
        scales = [jnp.exp2(top - highest) for top in tops]
        whole = sum(scale * total for scale, total in zip(scales, totals))
        weights = [scale / whole for scale in scales]
        padding = (-len(weights)) % 8
        square = jnp.concatenate(weights + [jnp.zeros((padding, rows), f32)] * (padding > 0), axis=0)
        columns = jnp.transpose(square)
        read = jnp.zeros((rows, HD), f32)
        for i, p in enumerate(parts):
            read = read + columns[:, i : i + 1] * p[:rows, cols].astype(f32)
        out_read.append((read * silu(gate_ref[part * rows : (part + 1) * rows, cols])).astype(bf16))
    out_read = out_read[0] if len(out_read) == 1 else jnp.concatenate(out_read, axis=1)
    partial = jnp.dot(
        mix_ref[part * rows : (part + 1) * rows, :], w_mix_ref[...], preferred_element_type=f32) + jnp.dot(
        out_read, w_read_ref[...], preferred_element_type=f32
    )
    whole_ref[...] = partial.astype(bf16)
    here = lax.axis_index("tp")
    share_rows = rows // shares
    for k in range(shares):
        start = pl.multiple_of((jnp.bitwise_xor(here, k) % shares) * share_rows, share_rows)
        outs[k][...] = whole_ref[pl.ds(start, share_rows), :]


def finish(parts, gate_read, out_mix, w_out_mix, w_out_read, shares, part):
    rows = out_mix.shape[0] // 2
    model = w_out_mix.shape[1]
    share = jax.ShapeDtypeStruct((rows // shares, model), bf16)
    return pl.pallas_call(
        functools.partial(finish_kernel, owners=len(parts), shares=shares, part=part),
        out_shape=[share] * shares,
        in_specs=[pl.BlockSpec(memory_space=pltpu.VMEM)] * (len(parts) + 4),
        out_specs=[pl.BlockSpec(memory_space=pltpu.VMEM)] * shares,
        scratch_shapes=[pltpu.VMEM((rows, model), bf16)],
        cost_estimate=pl.CostEstimate(
            flops=2 * rows * model * (w_out_mix.shape[0] + w_out_read.shape[0]),
            transcendentals=gate_read.size,
            bytes_accessed=2 * (w_out_mix.size + w_out_read.size + rows * model),
        ),
        name="finish",
    )(*parts, gate_read, out_mix, w_out_mix, w_out_read)


def shifted_by(value, axis, step):
    count = lax.axis_size(axis)
    if step % count == 0:
        return value
    return lax.ppermute(value, axis, [(i, (i + step) % count) for i in range(count)])


def crossed_by(value, axis, mask):
    if mask == 0:
        return value
    return lax.ppermute(value, axis, [(i, i ^ mask) for i in range(lax.axis_size(axis))])


def local(
    tokens,
    pre_gain,
    w_gated,
    w_mixed,
    mix_weight,
    w_query,
    w_gate_mix,
    w_gate_read,
    store,
    mem_gain,
    w_key,
    w_value,
    passage_ids,
    w_out_mix,
    w_out_read,
):
    readers = lax.axis_size("st")
    near = lax.axis_size("tp") // 2
    held = store.shape[0]
    first = (1 - lax.axis_index("tp") // near).astype(jnp.int32).reshape(1)
    normed, query = make_queries(first, passage_ids, tokens, pre_gain, w_query, held)
    queries = [shifted_by(query, "st", k) for k in range(readers)]
    keys, values = project_store(store, mem_gain, w_key, w_value)
    gate_mix = jnp.dot(normed, w_gate_mix, preferred_element_type=f32)
    arrived = []
    for part in range(2):
        reads = attend(queries, keys, values, held, part)
        if part == 0:
            reads, normed = lax.optimization_barrier((reads, normed))
        reads = [shifted_by(reads[k], "st", -k) for k in range(readers)]
        if part == 0:
            gated = jnp.dot(normed, w_gated, preferred_element_type=f32)
            mixed_in = jnp.dot(normed, w_mixed, preferred_element_type=f32)
            gate_read = jnp.dot(normed, w_gate_read, preferred_element_type=f32)
            out_mix = mix(mixed_in, gated, gate_mix, mix_weight)
        chunks = finish(reads, gate_read, out_mix, w_out_mix, w_out_read, near, part)
        base = near * (1 - part)
        if part == 0:
            chunks, queries = lax.optimization_barrier((chunks, queries))
        arrived += [crossed_by(chunks[k], "tp", base + k) for k in range(near)]
    return functools.reduce(jnp.add, [piece.astype(f32) for piece in arrived]).astype(bf16)


def solution(mesh):
    placed = (
        P(("grp", "st"), None),
        P(),
        P(None, "tp"),
        P(None, "tp"),
        P("tp", None, None),
        P(None, "tp"),
        P(None, "tp"),
        P(None, "tp"),
        P(("grp", "st"), None, None),
        P(),
        P(None, "tp"),
        P(None, "tp"),
        P(("grp", "st"), None),
        P("tp", None),
        P("tp", None),
    )
    return jax.shard_map(
        local, mesh=mesh, in_specs=placed, out_specs=P(("grp", "st", "tp"), None), check_vma=False
    )
```
